32 devices in a mesh: fs: 8 (over z, y), tp: 4 (over x, core).
Axes of the slice: x: 2, y: 2, z: 4, core: 2. Of those that a mesh axis runs over, the one named last changes fastest.
Arguments:
- rnn_out: bfloat16 [6144, 1536], P('fs', 'tp'), may hold values from -6 to 6
- out_grad: bfloat16 [6144, 2048], P('fs', 'tp'), may hold values from -0.109375 to 0.109375
- weight: float32 [2048, 1536], P('fs', 'tp'), may hold values from -0.15625 to 0.15625
- left_root: bfloat16 [4, 2048, 2048], P('tp', 'fs'), as said below
- right_root: bfloat16 [4, 384, 384], P('tp'), as said below
- left_stat: float32 [4, 2048, 2048], P('tp', 'fs'), may hold values from -4 to 4
- right_stat: float32 [4, 384, 384], P('tp', 'fs'), may hold values from -4 to 4
Outputs:
- new_weight: float32 [2048, 1536], P('fs', 'tp')
- step: float32 [2048, 1536], P('fs', 'tp')
- left_new: float32 [4, 2048, 2048], P('tp', 'fs')
- right_new: float32 [4, 384, 384], P('tp', 'fs')
- weight_copy: bfloat16 [2048, 1536], P(None, 'tp')
The draws below stay inside these ranges and needn't reach their ends.
Inputs may be any that keep to these rules, and one draw needn't show every extreme that they name: `left_root`: each block is symmetric. `right_root`: each block is symmetric.
All inputs are finite; a program needn't handle non-finite values.
Results may differ from the reference program's by a relative error of at most 0.0049.
Values may be sent and summed in bfloat16 or wider, within the bound.
A program may use at most 64 MiB of HBM per device.

```python
import jax
import jax.numpy as jnp

D = 2048
R = 1536
TOKENS = 6144
NB = 4
RB = 384


def symmetric_root(key, width):
    noise = jax.random.normal(key, (NB, width, width), jnp.float32)
    mixed = (noise + jnp.swapaxes(noise, 1, 2)) * (0.5 / (2.0 * width) ** 0.5)
    matrix = jnp.eye(width, dtype=jnp.float32)[None] + mixed
    return matrix


def draw_left_root(key, part):
    return symmetric_root(jax.random.fold_in(key, 11), D).astype(jnp.bfloat16)


def draw_right_root(key, part):
    return symmetric_root(jax.random.fold_in(key, 23), RB).astype(jnp.bfloat16)


def spiked(values, own_key, source, target, blocks, factor):
    def block_of(position):
        return (jnp.arange(values.shape[position]) // (values.shape[position] // blocks)).reshape((-1,) + (1,) * (values.ndim - 1 - position))

    first = jax.random.permutation(own_key, blocks)[block_of(target)]
    second = (block_of(target) + blocks // 2) % blocks
    return jnp.where((block_of(source) == first) | (block_of(source) == second), factor * values, values)


def block_levels(rng, shape, cuts, smallest, top_value):
    def one(position, shards_of):
        heights = jax.random.uniform(jax.random.fold_in(jax.random.fold_in(rng, 6), position), (shards_of,), jnp.float32, smallest / len(cuts), top_value / len(cuts))
        return jnp.repeat(jnp.exp(heights), shape[position] // shards_of).reshape((-1,) + (1,) * (len(shape) - position - 1))

    factor_of = one(*cuts[0])
    for cut in cuts[1:]:
        factor_of = factor_of * one(*cut)
    return factor_of


def normal_values(own_key, extent, scale, most, split=(), kind=jnp.bfloat16):
    result = scale * jax.random.normal(own_key, extent, jnp.float32)
    if split:
        result = result * block_levels(own_key, extent, split, -0.22, 0.18)
    return jnp.clip(result, -most, most).astype(kind)


def heavy_noise(rng, extent, scale, reach, pieces, heavy, kind=jnp.bfloat16):
    entries = scale * jax.random.normal(rng, extent, jnp.float32)
    if pieces:
        entries = entries * block_levels(rng, extent, pieces, -0.22, 0.18)
    return jnp.clip(spiked(entries, jax.random.fold_in(rng, 3), *heavy), -reach, reach).astype(kind)


def setup_inputs(seed: int = 0) -> dict:
    streams_of = jax.random.split(jax.random.key(seed), 8)
    rnn_out = normal_values(streams_of[0], (TOKENS, R), 1.0, 6.0, ((0, 8), (1, 4)))
    out_grad = heavy_noise(streams_of[1], (TOKENS, D), (1.0 / TOKENS ** 0.5), 0.109375, ((0, 8), (1, 4)), (0, 1, 8, 2.0))
    weight = normal_values(streams_of[2], (D, R), R ** -0.5, 0.15625, ((0, 8), (1, 4)), jnp.float32)
    left_root = draw_left_root(jax.random.fold_in(streams_of[7], 71), 0)
    right_root = draw_right_root(jax.random.fold_in(streams_of[7], 71), 0)
    left_stat = normal_values(streams_of[5], (NB, D, D), 0.5, 4.0, ((0, 4), (1, 8)), jnp.float32)
    right_stat = normal_values(streams_of[6], (NB, RB, RB), 0.5, 4.0, ((0, 4), (1, 8)), jnp.float32)
    return dict(rnn_out=rnn_out, out_grad=out_grad, weight=weight, left_root=left_root, right_root=right_root, left_stat=left_stat, right_stat=right_stat)


decay_rate = 0.8
step_size = 0.005

def reference(rnn_out, out_grad, weight, left_root, right_root, left_stat, right_stat):
    grad = jnp.dot(out_grad.T, rnn_out, preferred_element_type=jnp.float32)
    grad_low = grad.astype(jnp.bfloat16)
    grad_square = jnp.sum(grad * grad)
    lefts = []
    rights = []
    updates = []
    for index in range(NB):
        column = grad_low[:, index * RB:(index + 1) * RB]
        outer = jnp.dot(column, column.T, preferred_element_type=jnp.float32) / RB
        inner = jnp.dot(column.T, column, preferred_element_type=jnp.float32) / D
        lefts.append(decay_rate * left_stat[index] + (1.0 - decay_rate) * outer)
        rights.append(decay_rate * right_stat[index] + (1.0 - decay_rate) * inner)
        applied = jnp.dot(left_root[index], column, preferred_element_type=jnp.float32).astype(jnp.bfloat16)
        updates.append(jnp.dot(applied, right_root[index], preferred_element_type=jnp.float32))
    update = jnp.concatenate(updates, axis=1)
    scale = jnp.sqrt(grad_square + 1.0) / jnp.sqrt(jnp.sum(update * update) + 1.0)
    step = scale * update
    new_weight = weight - step_size * step
    return (new_weight, step, jnp.stack(lefts), jnp.stack(rights), new_weight.astype(jnp.bfloat16))
```

```python
import functools

import jax
import jax.numpy as jnp
from jax import lax
from jax.experimental import pallas as pl
from jax.experimental.pallas import tpu as pltpu
from jax.sharding import PartitionSpec as P

decay_rate = 0.8
step_size = 0.005


def body(rnn_out, out_grad, weight, left_root, right_root, left_stat, right_stat):
    block = weight.shape[1]
    width = left_root.shape[2]
    right_rows = right_stat.shape[1]
    right_start = lax.axis_index("fs") * right_rows
    cotangent = lax.all_gather(out_grad, "tp", axis=1, tiled=True)
    grad = lax.psum_scatter(
        lax.dot_general(
            cotangent, rnn_out, (((0,), (0,)), ((), ())), preferred_element_type=jnp.float32
        ),
        "fs",
        scatter_dimension=0,
        tiled=True,
    )
    grad_low = grad.astype(jnp.bfloat16)
    piece = lax.all_gather(grad_low, "fs", axis=0, tiled=True)
    root_columns = left_root[0]
    left_sum = jnp.dot(root_columns, piece, preferred_element_type=jnp.float32)
    own_columns = lax.dynamic_slice_in_dim(piece, right_start, right_rows, 1)
    right_sum = lax.dot_general(
        own_columns, piece, (((0,), (0,)), ((), ())), preferred_element_type=jnp.float32
    )
    product = lax.dot_general(
        grad_low, piece, (((1,), (1,)), ((), ())), preferred_element_type=jnp.float32
    )
    outer = product
    left_sum, right_sum, outer = (left_sum, right_sum, outer)
    grad_square = jnp.sum(grad * grad)
    total_grad = lax.psum(grad_square, ("fs", "tp"))
    left_new = decay_rate * left_stat + (1.0 - decay_rate) * (outer / block)[None]
    right_new = decay_rate * right_stat + (1.0 - decay_rate) * (right_sum / width)[None]
    applied = left_sum.astype(jnp.bfloat16)
    update = jnp.dot(applied, right_root[0], preferred_element_type=jnp.float32)
    update_square = jnp.sum(update * update)
    total_update = lax.psum(update_square, ("fs", "tp"))
    scale = jnp.sqrt(total_grad + 1.0) / jnp.sqrt(total_update + 1.0)
    step = scale * update
    new_weight = weight - step_size * step
    weight_copy = lax.all_gather(new_weight.astype(jnp.bfloat16), "fs", axis=0, tiled=True)
    return (new_weight, step, left_new, right_new, weight_copy)

MESH = pl.DeviceIdType.MESH
HALVES = 2


def dot(a, b, contract):
    return lax.dot_general(a, b, ((contract[:1], contract[1:]), ((), ())), preferred_element_type=jnp.float32)


def kernel(nf, nt, rnn, own, weight, root_hbm, right_root, stat_hbm, right_stat,
           new_weight, step, left_hbm, right_new, copy_out,
           root, stat, left, from_x, from_core, forwarded, pair_send, pair_recv, kept,
           line_send, line_recv, total, piece, applied_sum, inner, sums,
           local_sem, ax_s, ax_r, ac_s, ac_r, af_s, af_r, py_s, py_r, pz_s, pz_r,
           gz_s, gz_r, gy_s, gy_r, wz_s, wz_r, wy_s, wy_r, s_s, s_r):
    ny = 2
    nz = nf // ny
    count = nf * nt
    rows, block = weight.shape
    width = root.shape[1]
    half = rows // HALVES
    f, t = lax.axis_index("fs"), lax.axis_index("tp")
    me = f * nt + t
    z, y = f // ny, f % ny
    x, core = t // 2, t % 2
    other_y = 1 - y
    partner = {"fs": z * ny + other_y, "tp": t}
    over_x = {"fs": f, "tp": (1 - x) * 2 + core}
    over_core = {"fs": f, "tp": x * 2 + 1 - core}

    def remote(src, dst, send, recv, device):
        return pltpu.make_async_remote_copy(
            src_ref=src, dst_ref=dst, send_sem=send, recv_sem=recv, device_id=device, device_id_type=MESH
        )

    def peer(k):
        flat = (me + k) % count
        return {"fs": flat // nt, "tp": flat % nt}

    load_root = pltpu.make_async_copy(root_hbm, root, local_sem.at[0])
    load_stat = pltpu.make_async_copy(stat_hbm, stat, local_sem.at[1])
    load_root.start()
    load_stat.start()

    barrier = pltpu.get_barrier_semaphore()

    def greet(k, carry):
        pl.semaphore_signal(barrier, inc=1, device_id=peer(k), device_id_type=MESH)
        return carry

    lax.fori_loop(1, count, greet, 0)
    pl.semaphore_wait(barrier, count - 1)

    def own_chunk(k):
        c = other_y if k == 0 else y
        return own.at[:, pl.ds(pl.multiple_of(c * rows, rows), rows)]

    x_copies, core_copies, forward_copies, pair_copies = [], [], [], []
    for k in range(2):
        x_copies.append(remote(own_chunk(k), from_x.at[k], ax_s.at[k], ax_r.at[k], over_x))
        core_copies.append(remote(own_chunk(k), from_core.at[k], ac_s.at[k], ac_r.at[k], over_core))
        forward_copies.append(remote(from_x.at[k], forwarded.at[k], af_s.at[k], af_r.at[k], over_core))
    for k in range(2):
        x_copies[k].start()
        core_copies[k].start()
    for s in range(nt):
        pair_copies.append(remote(pair_send.at[s], pair_recv.at[s], py_s.at[s], py_r.at[s], partner))

    owners = [t, x * 2 + 1 - core, (1 - x) * 2 + core, (1 - x) * 2 + 1 - core]

    def line_copy(s):
        slot = (owners[s] - z + nz) % nz - 1
        return remote(line_send.at[s], line_recv.at[slot], pz_s.at[s], pz_r.at[slot],
                      {"fs": owners[s] * ny + y, "tp": t})

    def multiply(s, k, chunk):
        product = dot(chunk[...], rnn[...], (0, 0))
        if k == 0:
            pair_send[s] = product.astype(jnp.bfloat16)
            pair_copies[s].start()
        else:
            kept[s] = product

    def combine(s):
        pair_copies[s].wait_recv()
        both = kept[s] + pair_recv[s].astype(jnp.float32)

        @pl.when(owners[s] == z)
        def _():
            total[...] = both

        @pl.when(owners[s] != z)
        def _():
            line_send[s] = both.astype(jnp.bfloat16)
            line_copy(s).start()

    for k in range(2):
        multiply(0, k, own_chunk(k))
    for k in range(2):
        core_copies[k].wait_recv()
        multiply(1, k, from_core.at[k])
    combine(0)
    for k in range(2):
        x_copies[k].wait_recv()
        forward_copies[k].start()
        multiply(2, k, from_x.at[k])
        if k == 0:
            combine(1)
    for k in range(2):
        forward_copies[k].wait_recv()
        multiply(3, k, forwarded.at[k])
        if k == 0:
            combine(2)
    combine(3)

    def line_arrival(dz):
        return remote(line_send.at[0], line_recv.at[dz - 1], pz_s.at[0], pz_r.at[dz - 1], partner)

    for dz in range(1, nz):
        line_arrival(dz).wait_recv()
        total[...] += line_recv[dz - 1].astype(jnp.float32)
    grad = total[...]
    sums[me, 0:8, :] = jnp.full((8, 128), jnp.sum(grad * grad))
    piece[f] = grad.astype(jnp.bfloat16)

    def gather(buffer, z_s, z_r, y_s, y_r, use):
        def part(owner, h):
            return buffer.at[owner, pl.ds(h * half, half)]

        def along(dz, h):
            return remote(part(f, h), part(f, h), z_s.at[dz - 1, h], z_r.at[dz - 1, h],
                          {"fs": (z + dz) % nz * ny + y, "tp": t})

        def source(dz, side):
            return (z - dz + nz) % nz * ny + side

        def arrival(dz, h):
            mine = part(source(dz, y), h)
            return remote(mine, mine, z_s.at[dz - 1, h], z_r.at[dz - 1, h], partner)

        def across(dz, h):
            mine = part(source(dz, y), h)
            return remote(mine, mine, y_s.at[dz, h], y_r.at[dz, h], partner)

        def crossed(dz, h):
            theirs = part(source(dz, other_y), h)
            return remote(theirs, theirs, y_s.at[dz, h], y_r.at[dz, h], partner)

        for dz in range(1, nz):
            for h in range(HALVES):
                along(dz, h).start()
                if dz == 1:
                    across(0, h).start()
        use(f)
        for dz in range(1, nz):
            for h in range(HALVES):
                arrival(dz, h).wait_recv()
                across(dz, h).start()
            use(source(dz, y))
            for h in range(HALVES):
                crossed(dz - 1, h).wait_recv()
            use(source(dz - 1, other_y))
        for h in range(HALVES):
            crossed(nz - 1, h).wait_recv()
        use(source(nz - 1, other_y))
        for dz in range(1, nz):
            for h in range(HALVES):
                along(dz, h).wait_send()
        for dz in range(nz):
            for h in range(HALVES):
                across(dz, h).wait_send()

    def columns(owner):
        return pl.ds(pl.multiple_of(owner * rows, rows), rows)

    load_root.wait()
    load_stat.wait()
    applied_sum[...] = jnp.zeros_like(applied_sum)

    def apply_left(owner):
        applied_sum[...] += dot(root[:, columns(owner)], piece[owner], (1, 0))

    gather(piece, gz_s, gz_r, gy_s, gy_r, apply_left)

    update = dot(applied_sum[...].astype(jnp.bfloat16), right_root[...], (1, 0))
    step[...] = update
    sums[me, 8:16, :] = jnp.full((8, 128), jnp.sum(update * update))

    def sum_copy(k):
        return remote(sums.at[me], sums.at[me], s_s.at[k], s_r.at[k], peer(k))

    def sum_arrival(k):
        theirs = sums.at[(me - k + count) % count]
        return remote(theirs, theirs, s_s.at[k], s_r.at[k], peer(k))

    def send_sum(k, carry):
        sum_copy(k).start()
        return carry

    def take_sum(k, carry):
        sum_arrival(k).wait_recv()
        return carry

    def end_sum(k, carry):
        sum_copy(k).wait_send()
        return carry

    lax.fori_loop(1, count, send_sum, 0)
    inner[...] = jnp.zeros_like(inner)
    for owner in range(nf):
        inner[...] += dot(piece[owner], piece[owner], (0, 0))
    lax.fori_loop(1, count, take_sum, 0)
    everything = jnp.sum(sums[...], axis=0)
    scale = jnp.sqrt(everything[0:1, 0:1] + 1.0) / jnp.sqrt(everything[8:9, 0:1] + 1.0)
    scaled = scale * step[...]
    step[...] = scaled
    fresh = weight[...] - step_size * scaled
    new_weight[...] = fresh
    copy_out[f] = fresh.astype(jnp.bfloat16)

    def left_block(owner):
        product = dot(piece[f], piece[owner], (1, 1))
        left[:, columns(owner)] = decay_rate * stat[:, columns(owner)] + (1.0 - decay_rate) * (product / block)

    gather(copy_out, wz_s, wz_r, wy_s, wy_r, left_block)
    store_left = pltpu.make_async_copy(left, left_hbm, local_sem.at[2])
    store_left.start()
    right_rows = right_stat.shape[0]
    inner_rows = inner[pl.ds(pl.multiple_of(f * right_rows, 8), right_rows), :]
    right_new[...] = decay_rate * right_stat[...] + (1.0 - decay_rate) * (inner_rows / width)

    lax.fori_loop(1, count, end_sum, 0)
    for k in range(2):
        x_copies[k].wait_send()
        core_copies[k].wait_send()
        forward_copies[k].wait_send()
    for s in range(nt):
        pair_copies[s].wait_send()

        @pl.when(owners[s] != z)
        def _():
            line_copy(s).wait_send()

    store_left.wait()


def kernel_body(nf, nt, rnn_out, out_grad, weight, left_root, right_root, left_stat, right_stat):
    rows, block = weight.shape
    tokens = rnn_out.shape[0]
    width = left_root.shape[2]
    right_rows = right_stat.shape[1]
    nz = nf // 2
    low, full = jnp.bfloat16, jnp.float32
    vmem = pl.BlockSpec(memory_space=pltpu.VMEM)
    hbm = pl.BlockSpec(memory_space=pl.ANY)
    dma = pltpu.SemaphoreType.DMA
    out = pl.pallas_call(
        functools.partial(kernel, nf, nt),
        out_shape=(
            jax.ShapeDtypeStruct((rows, block), full),
            jax.ShapeDtypeStruct((rows, block), full),
            jax.ShapeDtypeStruct((rows, width), full),
            jax.ShapeDtypeStruct((right_rows, block), full),
            jax.ShapeDtypeStruct((nf, rows, block), low),
        ),
        in_specs=[vmem, vmem, vmem, hbm, vmem, hbm, vmem],
        out_specs=(vmem, vmem, hbm, vmem, vmem),
        scratch_shapes=[
            pltpu.VMEM((rows, width), low),
            pltpu.VMEM((rows, width), full),
            pltpu.VMEM((rows, width), full),
            pltpu.VMEM((2, tokens, rows), low),
            pltpu.VMEM((2, tokens, rows), low),
            pltpu.VMEM((2, tokens, rows), low),
            pltpu.VMEM((nt, rows, block), low),
            pltpu.VMEM((nt, rows, block), low),
            pltpu.VMEM((nt, rows, block), full),
            pltpu.VMEM((nt, rows, block), low),
            pltpu.VMEM((nz - 1, rows, block), low),
            pltpu.VMEM((rows, block), full),
            pltpu.VMEM((nf, rows, block), low),
            pltpu.VMEM((rows, block), full),
            pltpu.VMEM((block, block), full),
            pltpu.VMEM((nf * nt, 16, 128), full),
            dma((3,)),
            dma((2,)), dma((2,)), dma((2,)), dma((2,)), dma((2,)), dma((2,)),
            dma((nt,)), dma((nt,)), dma((nt,)), dma((nz - 1,)),
            dma((nz - 1, HALVES)), dma((nz - 1, HALVES)), dma((nz, HALVES)), dma((nz, HALVES)),
            dma((nz - 1, HALVES)), dma((nz - 1, HALVES)), dma((nz, HALVES)), dma((nz, HALVES)),
            dma((nf * nt,)), dma((nf * nt,)),
        ],
        compiler_params=pltpu.CompilerParams(
            collective_id=0, has_side_effects=True, vmem_limit_bytes=60 * 1024 * 1024
        ),
    )(rnn_out, out_grad, weight, left_root[0], right_root[0], left_stat[0], right_stat[0])
    new_weight, step, left_new, right_new, weight_copy = out
    return new_weight, step, left_new[None], right_new[None], weight_copy.reshape(width, block)


def solution(mesh):
    placed = (
        P("fs", "tp"),
        P("fs", "tp"),
        P("fs", "tp"),
        P("tp", "fs", None),
        P("tp", None, None),
        P("tp", "fs", None),
        P("tp", "fs", None),
    )
    nf, nt = mesh.shape["fs"], mesh.shape["tp"]
    chosen = functools.partial(kernel_body, nf, nt) if nt == 4 and nf == 2 * nt else body
    return jax.shard_map(
        chosen,
        mesh=mesh,
        in_specs=placed,
        out_specs=(
            P("fs", "tp"),
            P("fs", "tp"),
            P("tp", "fs", None),
            P("tp", "fs", None),
            P(None, "tp"),
        ),
        check_vma=False,
    )
```

```python
import functools

import jax
import jax.numpy as jnp
from jax import lax
from jax.experimental import pallas as pl
from jax.experimental.pallas import tpu as pltpu
from jax.sharding import PartitionSpec as P

decay_rate = 0.8
step_size = 0.005


def body(rnn_out, out_grad, weight, left_root, right_root, left_stat, right_stat):
    block = weight.shape[1]
    width = left_root.shape[2]
    right_rows = right_stat.shape[1]
    right_start = lax.axis_index("fs") * right_rows
    cotangent = lax.all_gather(out_grad, "tp", axis=1, tiled=True)
    grad = lax.psum_scatter(
        lax.dot_general(
            cotangent, rnn_out, (((0,), (0,)), ((), ())), preferred_element_type=jnp.float32
        ),
        "fs",
        scatter_dimension=0,
        tiled=True,
    )
    grad_low = grad.astype(jnp.bfloat16)
    piece = lax.all_gather(grad_low, "fs", axis=0, tiled=True)
    root_columns = left_root[0]
    left_sum = jnp.dot(root_columns, piece, preferred_element_type=jnp.float32)
    own_columns = lax.dynamic_slice_in_dim(piece, right_start, right_rows, 1)
    right_sum = lax.dot_general(
        own_columns, piece, (((0,), (0,)), ((), ())), preferred_element_type=jnp.float32
    )
    product = lax.dot_general(
        grad_low, piece, (((1,), (1,)), ((), ())), preferred_element_type=jnp.float32
    )
    outer = product
    left_sum, right_sum, outer = (left_sum, right_sum, outer)
    grad_square = jnp.sum(grad * grad)
    total_grad = lax.psum(grad_square, ("fs", "tp"))
    left_new = decay_rate * left_stat + (1.0 - decay_rate) * (outer / block)[None]
    right_new = decay_rate * right_stat + (1.0 - decay_rate) * (right_sum / width)[None]
    applied = left_sum.astype(jnp.bfloat16)
    update = jnp.dot(applied, right_root[0], preferred_element_type=jnp.float32)
    update_square = jnp.sum(update * update)
    total_update = lax.psum(update_square, ("fs", "tp"))
    scale = jnp.sqrt(total_grad + 1.0) / jnp.sqrt(total_update + 1.0)
    step = scale * update
    new_weight = weight - step_size * step
    weight_copy = lax.all_gather(new_weight.astype(jnp.bfloat16), "fs", axis=0, tiled=True)
    return (new_weight, step, left_new, right_new, weight_copy)

MESH = pl.DeviceIdType.MESH
HALVES = 4


def dot(a, b, contract):
    return lax.dot_general(a, b, ((contract[:1], contract[1:]), ((), ())), preferred_element_type=jnp.float32)


def kernel(nf, nt, rnn_hbm, own_hbm, weight_hbm, root_hbm, right_root_hbm, stat_hbm, right_stat_hbm,
           new_weight, step, left, right_new, copy_out,
           rnn, weight, right_root, right_stat, root, stat, chip, far, pair_send, pair_recv, kept,
           line_send, line_recv, total, piece, applied_sum, inner, sums,
           local_sem, ax_s, ax_r, ac_s, ac_r, af_s, af_r, py_s, py_r, pz_s, pz_r,
           gz_s, gz_r, gy_s, gy_r, wz_s, wz_r, wy_s, wy_r, s_s, s_r):
    ny = 2
    nz = nf // ny
    count = nf * nt
    rows, block = weight.shape
    width = root.shape[1]
    half = rows // HALVES
    f, t = lax.axis_index("fs"), lax.axis_index("tp")
    me = f * nt + t
    z, y = f // ny, f % ny
    x, core = t // 2, t % 2
    other_y = 1 - y
    partner = {"fs": z * ny + other_y, "tp": t}
    over_x = {"fs": f, "tp": (1 - x) * 2 + core}
    over_core = {"fs": f, "tp": x * 2 + 1 - core}

    def remote(src, dst, send, recv, device):
        return pltpu.make_async_remote_copy(
            src_ref=src, dst_ref=dst, send_sem=send, recv_sem=recv, device_id=device, device_id_type=MESH
        )

    def peer(k):
        flat = (me + k) % count
        return {"fs": flat // nt, "tp": flat % nt}

    load_root = pltpu.make_async_copy(root_hbm, root, local_sem.at[0])
    load_stat = pltpu.make_async_copy(stat_hbm, stat, local_sem.at[1])
    load_own = []
    for k in range(2):
        chunk = pl.ds(pl.multiple_of((other_y if k == 0 else y) * rows, rows), rows)
        load_own.append(pltpu.make_async_copy(own_hbm.at[:, chunk], chip.at[core, k], local_sem.at[2 + k]))
        load_own[k].start()
    load_rnn = pltpu.make_async_copy(rnn_hbm, rnn, local_sem.at[4])
    later = [
        load_root,
        load_stat,
        pltpu.make_async_copy(weight_hbm, weight, local_sem.at[5]),
        pltpu.make_async_copy(right_root_hbm, right_root, local_sem.at[6]),
        pltpu.make_async_copy(right_stat_hbm, right_stat, local_sem.at[7]),
    ]
    load_rnn.start()
    for load in later:
        load.start()

    barrier = pltpu.get_barrier_semaphore()

    def greet(k, carry):
        pl.semaphore_signal(barrier, inc=1, device_id=peer(k), device_id_type=MESH)
        return carry

    lax.fori_loop(1, count, greet, 0)
    pl.semaphore_wait(barrier, count - 1)

    tokens = rnn.shape[0]
    split = tokens // 2
    share = pl.ds(pl.multiple_of(core * split, split), split)

    x_copies, core_copies, forward_copies, pair_copies = [], [], [], []
    for k in range(2):
        core_copies.append(remote(chip.at[core, k], chip.at[core, k], ac_s.at[k], ac_r.at[k], over_core))
    for i in range(4):
        holder = x if i < 2 else 1 - x
        mine = far.at[i, share]
        x_copies.append(remote(chip.at[holder, i % 2, share], mine, ax_s.at[i], ax_r.at[i], over_x))
        forward_copies.append(remote(mine, mine, af_s.at[i], af_r.at[i], over_core))

    def start_first():
        for i in range(2):
            x_copies[i].start()

    for k in range(2):
        load_own[k].wait()
        core_copies[k].start()
    pl.when(core == x)(start_first)
    for k in range(2):
        core_copies[k].wait_recv()
    pl.when(core != x)(start_first)
    for i in range(2, 4):
        x_copies[i].start()
    for s in range(nt):
        pair_copies.append(remote(pair_send.at[s], pair_recv.at[s], py_s.at[s], py_r.at[s], partner))

    owners = [t, x * 2 + 1 - core, (1 - x) * 2 + 1 - x, (1 - x) * 2 + x]

    def line_copy(s):
        slot = (owners[s] - z + nz) % nz - 1
        return remote(line_send.at[s], line_recv.at[slot], pz_s.at[s], pz_r.at[slot],
                      {"fs": owners[s] * ny + y, "tp": t})

    def multiply(s, k, chunk):
        product = dot(chunk[...], rnn[...], (0, 0))
        if k == 0:
            pair_send[s] = product.astype(jnp.bfloat16)
            pair_copies[s].start()
        else:
            kept[s] = product

    def combine(s):
        pair_copies[s].wait_recv()
        both = kept[s] + pair_recv[s].astype(jnp.float32)

        @pl.when(owners[s] == z)
        def _():
            total[...] = both

        @pl.when(owners[s] != z)
        def _():
            line_send[s] = both.astype(jnp.bfloat16)
            line_copy(s).start()

    load_rnn.wait()
    for load in later:
        load.wait()
    for k in range(2):
        multiply(0, k, chip.at[core, k])
    for k in range(2):
        multiply(1, k, chip.at[1 - core, k])
    for i in range(4):
        x_copies[i].wait_recv()
        forward_copies[i].start()
        forward_copies[i].wait_recv()
        multiply(2 + i // 2, i % 2, far.at[i])
        if i < 3:
            combine(i)
    combine(3)

    def line_arrival(dz):
        return remote(line_send.at[0], line_recv.at[dz - 1], pz_s.at[0], pz_r.at[dz - 1], partner)

    for dz in range(1, nz):
        line_arrival(dz).wait_recv()
        total[...] += line_recv[dz - 1].astype(jnp.float32)
    grad = total[...]
    grad_square = jnp.sum(grad * grad)
    piece[f] = grad.astype(jnp.bfloat16)

    def gather(buffer, z_s, z_r, y_s, y_r, use):
        def part(owner, h):
            return buffer.at[owner, pl.ds(h * half, half)]

        def block_at(way, d, side):
            return (z - way * d + nz) % nz * ny + side

        def slot(way, d):
            return d if way > 0 else nz + d

        def onward(way, d, h):
            mine = part(block_at(way, d, y), h)
            there = (z + way + nz) % nz * ny + y
            return remote(mine, mine, z_s.at[slot(way, d), h], z_r.at[slot(way, d + 1), h], {"fs": there, "tp": t})

        def arrival(way, d, h):
            mine = part(block_at(way, d, y), h)
            return remote(mine, mine, z_s.at[slot(way, d), h], z_r.at[slot(way, d), h], partner)

        def across(way, d, h, side):
            mine = part(block_at(way, d, side), h)
            return remote(mine, mine, y_s.at[slot(way, d), h], y_r.at[slot(way, d), h], partner)

        def comes(way, d):
            return z >= d if way > 0 else z + d < nz

        def goes(way):
            return z + 1 < nz if way > 0 else z >= 1

        for h in range(HALVES):
            for way in (1, -1):
                pl.when(goes(way))(onward(way, 0, h).start)
            across(1, 0, h, y).start()
        use(f)
        for d in range(1, nz):
            for h in range(HALVES):
                for way in (1, -1):
                    @pl.when(comes(way, d))
                    def _(way=way, h=h):
                        arrival(way, d, h).wait_recv()
                        if d + 1 < nz:
                            pl.when(goes(way))(onward(way, d, h).start)
                        across(way, d, h, y).start()
            for way in (1, -1):
                @pl.when(comes(way, d))
                def _(way=way):
                    use(block_at(way, d, y))
        for d in range(nz):
            for way in (1, -1):
                if d or way > 0:
                    @pl.when(comes(way, d))
                    def _(way=way, d=d):
                        for h in range(HALVES):
                            across(way, d, h, other_y).wait_recv()
                        use(block_at(way, d, other_y))
        for d in range(nz):
            for way in (1, -1):
                @pl.when(comes(way, d))
                def _(way=way, d=d):
                    for h in range(HALVES):
                        if d + 1 < nz:
                            pl.when(goes(way))(onward(way, d, h).wait_send)
                        if d or way > 0:
                            across(way, d, h, y).wait_send()

    def columns(owner):
        return pl.ds(pl.multiple_of(owner * rows, rows), rows)

    applied_sum[...] = jnp.zeros_like(applied_sum)

    def apply_left(owner):
        applied_sum[...] += dot(root[:, columns(owner)], piece[owner], (1, 0))

    gather(piece, gz_s, gz_r, gy_s, gy_r, apply_left)

    update = dot(applied_sum[...].astype(jnp.bfloat16), right_root[...], (1, 0))
    step[...] = update
    lane = lax.broadcasted_iota(jnp.int32, (1, 128), 1)
    sums[me] = jnp.where(lane < 64, grad_square, jnp.sum(update * update))

    def sum_copy(k):
        return remote(sums.at[me], sums.at[me], s_s.at[k], s_r.at[k], peer(k))

    def sum_arrival(k):
        theirs = sums.at[(me - k + count) % count]
        return remote(theirs, theirs, s_s.at[k], s_r.at[k], peer(k))

    def send_sum(k, carry):
        sum_copy(k).start()
        return carry

    def take_sum(k, carry):
        sum_arrival(k).wait_recv()
        return carry

    def end_sum(k, carry):
        sum_copy(k).wait_send()
        return carry

    lax.fori_loop(1, count, send_sum, 0)
    inner[...] = jnp.zeros_like(inner)
    for owner in range(nf):
        inner[...] += dot(piece[owner], piece[owner], (0, 0))
    lax.fori_loop(1, count, take_sum, 0)
    everything = jnp.sum(sums[...], axis=0)
    scale = jnp.sqrt(everything[0:1, 0:1] + 1.0) / jnp.sqrt(everything[0:1, 64:65] + 1.0)
    scaled = scale * step[...]
    step[...] = scaled
    fresh = weight[...] - step_size * scaled
    new_weight[...] = fresh
    copy_out[f] = fresh.astype(jnp.bfloat16)

    def left_block(owner):
        product = dot(piece[f], piece[owner], (1, 1))
        left[:, columns(owner)] = decay_rate * stat[:, columns(owner)] + (1.0 - decay_rate) * (product / block)

    gather(copy_out, wz_s, wz_r, wy_s, wy_r, left_block)
    right_rows = right_stat.shape[0]
    inner_rows = inner[pl.ds(pl.multiple_of(f * right_rows, 8), right_rows), :]
    right_new[...] = decay_rate * right_stat[...] + (1.0 - decay_rate) * (inner_rows / width)

    lax.fori_loop(1, count, end_sum, 0)
    for k in range(2):
        core_copies[k].wait_send()
    for i in range(4):
        x_copies[i].wait_send()
        forward_copies[i].wait_send()
    for s in range(nt):
        pair_copies[s].wait_send()

        @pl.when(owners[s] != z)
        def _():
            line_copy(s).wait_send()


def settle_kernel(count, *refs):
    ins, outs, held, sems = refs[:count], refs[count:2 * count], refs[2 * count:3 * count], refs[3 * count]
    order = sorted(range(count), key=lambda i: -ins[i].size)
    for i in order:
        pltpu.make_async_copy(ins[i], held[i], sems.at[0, i]).start()
    for i in order[::-1]:
        pltpu.make_async_copy(ins[i], held[i], sems.at[0, i]).wait()
        pltpu.make_async_copy(held[i], outs[i], sems.at[1, i]).start()
    for i in order:
        pltpu.make_async_copy(held[i], outs[i], sems.at[1, i]).wait()


def settle(arrays):
    count = len(arrays)
    hbm = pl.BlockSpec(memory_space=pl.ANY)
    return pl.pallas_call(
        functools.partial(settle_kernel, count),
        out_shape=tuple(jax.ShapeDtypeStruct(a.shape, a.dtype) for a in arrays),
        in_specs=[hbm] * count,
        out_specs=(hbm,) * count,
        scratch_shapes=[pltpu.VMEM(a.shape, a.dtype) for a in arrays] + [pltpu.SemaphoreType.DMA((2, count))],
        compiler_params=pltpu.CompilerParams(vmem_limit_bytes=58 * 1024 * 1024),
    )(*arrays)


def kernel_body(nf, nt, rnn_out, out_grad, weight, left_root, right_root, left_stat, right_stat):
    rows, block = weight.shape
    tokens = rnn_out.shape[0]
    width = left_root.shape[2]
    right_rows = right_stat.shape[1]
    nz = nf // 2
    low, full = jnp.bfloat16, jnp.float32
    vmem = pl.BlockSpec(memory_space=pltpu.VMEM)
    hbm = pl.BlockSpec(memory_space=pltpu.HBM)
    dma = pltpu.SemaphoreType.DMA
    out = pl.pallas_call(
        functools.partial(kernel, nf, nt),
        out_shape=(
            jax.ShapeDtypeStruct((rows, block), full),
            jax.ShapeDtypeStruct((rows, block), full),
            jax.ShapeDtypeStruct((rows, width), full),
            jax.ShapeDtypeStruct((right_rows, block), full),
            jax.ShapeDtypeStruct((nf, rows, block), low),
        ),
        in_specs=[hbm] * 7,
        out_specs=(vmem,) * 5,
        scratch_shapes=[
            pltpu.VMEM((tokens, block), low),
            pltpu.VMEM((rows, block), full),
            pltpu.VMEM((block, block), low),
            pltpu.VMEM((right_rows, block), full),
            pltpu.VMEM((rows, width), low),
            pltpu.VMEM((rows, width), full),
            pltpu.VMEM((2, 2, tokens, rows), low),
            pltpu.VMEM((4, tokens, rows), low),
            pltpu.VMEM((nt, rows, block), low),
            pltpu.VMEM((nt, rows, block), low),
            pltpu.VMEM((nt, rows, block), full),
            pltpu.VMEM((nt, rows, block), low),
            pltpu.VMEM((nz - 1, rows, block), low),
            pltpu.VMEM((rows, block), full),
            pltpu.VMEM((nf, rows, block), low),
            pltpu.VMEM((rows, block), full),
            pltpu.VMEM((block, block), full),
            pltpu.VMEM((nf * nt, 1, 128), full),
            dma((8,)),
            dma((4,)), dma((4,)), dma((2,)), dma((2,)), dma((4,)), dma((4,)),
            dma((nt,)), dma((nt,)), dma((nt,)), dma((nz - 1,)),
            dma((2 * nz, HALVES)), dma((2 * nz, HALVES)), dma((2 * nz, HALVES)), dma((2 * nz, HALVES)),
            dma((2 * nz, HALVES)), dma((2 * nz, HALVES)), dma((2 * nz, HALVES)), dma((2 * nz, HALVES)),
            dma((nf * nt,)), dma((nf * nt,)),
        ],
        compiler_params=pltpu.CompilerParams(
            collective_id=0, has_side_effects=True, vmem_limit_bytes=58 * 1024 * 1024
        ),
    )(rnn_out, out_grad, weight, left_root[0], right_root[0], left_stat[0], right_stat[0])
    new_weight, step, left_new, right_new, weight_copy = settle(out)
    return new_weight, step, left_new[None], right_new[None], weight_copy.reshape(width, block)


def solution(mesh):
    placed = (
        P("fs", "tp"),
        P("fs", "tp"),
        P("fs", "tp"),
        P("tp", "fs", None),
        P("tp", None, None),
        P("tp", "fs", None),
        P("tp", "fs", None),
    )
    nf, nt = mesh.shape["fs"], mesh.shape["tp"]
    chosen = functools.partial(kernel_body, nf, nt) if nt == 4 and nf == 2 * nt else body
    return jax.shard_map(
        chosen,
        mesh=mesh,
        in_specs=placed,
        out_specs=(
            P("fs", "tp"),
            P("fs", "tp"),
            P("tp", "fs", None),
            P("tp", "fs", None),
            P(None, "tp"),
        ),
        check_vma=False,
    )
```
